1024 devices in a mesh: ep: 64 (over z, y), tp: 16 (over x, core).
Axes of the slice: x: 8, y: 8, z: 8, core: 2. Of those that a mesh axis runs over, the one named last changes fastest.
Arguments:
- tokens: bfloat16 [8192, 2048], P('ep'), may hold values from -6 to 6
- cotangent: bfloat16 [8192, 2048], P('ep'), may hold values from -0.796875 to 0.796875
- mix_weights: bfloat16 [8192, 2], P('ep'), may hold values from 0.049804688 to 1
- routes: int32 [8192, 2], P('ep'), may hold values from 0 to 63, all different within a row; in each aligned block of 128 rows (0 to 127, 128 to 255, ...) at most 5 rows name the same one
- gate_proj: bfloat16 [64, 2048, 2048], P('ep', None, 'tp'), may hold values from -0.125 to 0.125
- up_proj: bfloat16 [64, 2048, 2048], P('ep', None, 'tp'), may hold values from -0.125 to 0.125
- down_proj: bfloat16 [64, 2048, 2048], P('ep', 'tp'), may hold values from -0.125 to 0.125
Outputs:
- token_grad: bfloat16 [8192, 2048], P('ep', 'tp')
- mix_grad: bfloat16 [8192, 2], P('ep')
- gate_grad: bfloat16 [64, 2048, 2048], P('ep', None, 'tp')
- up_grad: bfloat16 [64, 2048, 2048], P('ep', None, 'tp')
- down_grad: bfloat16 [64, 2048, 2048], P('ep', 'tp')
The draws below stay inside these ranges and needn't reach their ends.
Inputs may be any that keep to these rules, and one draw needn't show every extreme that they name: `routes`: each row names 2 different experts; in each aligned block of 128 rows (the rows of one device) no expert is named more than 5 times, a bound that some block reaches.
All inputs are finite; a program needn't handle non-finite values.
Results may differ from the reference program's by a relative error of at most 0.018.
Values may be sent and summed in bfloat16 or wider, within the bound.
No kernel may reach another device: no remote copies, remote signals or barrier semaphores. Data moves between devices by JAX's collectives and lax.ppermute only.
A program may use at most 128 MiB of HBM per device.

```python
import math
import jax
import jax.numpy as jnp
import numpy as np
from jax import lax

D = 2048
FF = 2048
TOPK = 2
TOK_DEV = 128
EXPERTS = 64
TOKENS = 8192
CAP = 5
FF_DEV = 128
N_EP = 64
N_TP = 16


def steps_of(rng, shape, shards, low, top_value):
    loudness = 1.0
    for dim, shards_of in shards:
        heights = jax.random.uniform(jax.random.fold_in(jax.random.fold_in(rng, 6), dim), (shards_of,), jnp.float32, low / len(shards), top_value / len(shards))
        loudness = loudness * jnp.repeat(jnp.exp(heights), shape[dim] // shards_of).reshape((-1,) + (1,) * (len(shape) - 1 - dim))
    return loudness


def routed_block(own_key, own, number, rows, count, top, bound, slope):
    order = jax.random.permutation(own_key, count)
    heavy_load, usual = portions_of(count, rows * top, bound, slope, True), portions_of(count, rows * top, bound, slope, False)
    places = jnp.arange(count)

    def named(lengths, rotation):
        used = int((lengths > 0).sum())
        fixed = max(1, used // 4)
        shifted = fixed + (places - fixed + rotation * (used - fixed)) % max(1, count - fixed)
        return jnp.zeros((count,), jnp.int32).at[order[jnp.where(places < fixed, places, shifted)]].set(jnp.asarray(lengths, jnp.int32))

    lengths = jnp.where(number % 4 == 0, named(heavy_load, number // 4), named(usual, number - number // 4 - 1))
    mixed = jax.random.permutation(jax.random.fold_in(own, 3), count)
    giver, taker = mixed[0:count // 2 * 2:2], mixed[1:count // 2 * 2:2]
    room = jnp.minimum(lengths[giver] - 1, bound - lengths[taker]) // 2
    room = jnp.where((giver == order[0]) | (taker == order[0]) | (lengths[taker] == 0), 0, jnp.maximum(room, 0))
    shifted = jax.random.randint(jax.random.fold_in(own, 4), (count // 2,), 0, 1 << 20) % (room + 1)
    lengths = lengths.at[giver].add(-shifted).at[taker].add(shifted)
    labels = jnp.searchsorted(jnp.cumsum(lengths), jnp.arange(rows * top), side="right").astype(jnp.int32)
    listing = labels.reshape(top, rows).T
    listing = listing[jax.random.permutation(jax.random.fold_in(own, 1), rows)]
    rotation = jax.random.randint(jax.random.fold_in(own, 2), (rows, 1), 0, top)
    return jnp.take_along_axis(listing, (jnp.arange(top)[None, :] + rotation) % top, axis=1)


def portions_of(amount, total, reach, slope, full):
    loads = [(1 << 20) // math.isqrt(rank ** slope) + 1 for rank in range(1, amount + 1)]
    largest = reach if full else min(reach, max(-(-total // amount), total * loads[0] // sum(loads)))
    least = 1 if total - largest >= amount - 1 else 0
    counts, spare = [largest] + [least] * (amount - 1), total - largest - least * (amount - 1)
    while spare > 0:
        candidates = [i for i in range(1, amount) if counts[i] < largest] or [i for i in range(1, amount) if counts[i] < reach]
        pool, budget = sum([loads[i] for i in candidates]), spare
        for i in candidates:
            addition = min(reach - counts[i], max(1, budget * loads[i] // pool), spare)
            counts[i] = counts[i] + addition
            spare = spare - addition
    return np.array(counts)


def noise(stream_key, shape, deviation, bound, split=(), kind=jnp.bfloat16):
    result = deviation * jax.random.normal(stream_key, shape, jnp.float32)
    if split:
        result = result * steps_of(stream_key, shape, split, -0.22, 0.18)
    return jnp.clip(result, -bound, bound).astype(kind)


def setup_inputs(seed: int = 0) -> dict:
    arg_keys = jax.random.split(jax.random.key(seed), 8)
    tokens = noise(arg_keys[0], (TOKENS, D), 1.0, 6.0, ((0, 64),))
    cotangent = noise(arg_keys[1], (TOKENS, D), 0.1, 0.796875, ((0, 64),))
    mix_weights = jnp.clip(jnp.exp(math.log(1.0) - 2.9996462 * jax.random.uniform(arg_keys[2], (TOKENS, TOPK), jnp.float32) ** steps_of(arg_keys[2], (TOKENS, TOPK), ((0, 64),), -0.2, 0.2)), 0.049804688, 1.0).astype(jnp.bfloat16)
    routes_keys = jax.random.split(jax.random.fold_in(arg_keys[3], 1), TOKENS // TOK_DEV)
    routes_turns = jax.random.permutation(jax.random.fold_in(arg_keys[3], 3), TOKENS // TOK_DEV)
    routes = jax.vmap(lambda own, number: routed_block(jax.random.fold_in(arg_keys[3], 2), own, number, TOK_DEV, EXPERTS, TOPK, CAP, 1))(routes_keys, routes_turns).reshape((TOKENS, TOPK))
    gate_proj = noise(arg_keys[4], (EXPERTS, D, FF), D ** -0.5, 0.125, ((0, 64), (2, 16)))
    up_proj = noise(arg_keys[5], (EXPERTS, D, FF), D ** -0.5, 0.125, ((0, 64), (2, 16)))
    down_proj = noise(arg_keys[6], (EXPERTS, FF, D), FF ** -0.5, 0.125, ((0, 64), (1, 16)))
    return {"tokens": tokens, "cotangent": cotangent, "mix_weights": mix_weights, "routes": routes, "gate_proj": gate_proj, "up_proj": up_proj, "down_proj": down_proj}


def silu_slope(pre):
    sig = jax.nn.sigmoid(pre)
    return sig * (1.0 + pre * (1.0 - sig))


def pair_table(routes):
    pairs = TOKENS * TOPK
    flat = routes.reshape(-1).astype(jnp.int32)
    onehot = (flat[:, None] == jnp.arange(EXPERTS, dtype=jnp.int32)[None, :]).astype(jnp.int32)
    blocks = onehot.reshape(N_EP, TOK_DEV * TOPK, EXPERTS)
    before = jnp.cumsum(blocks, axis=1) - blocks
    rank = jnp.sum(before * blocks, axis=2).reshape(-1).astype(jnp.int32)
    source = jnp.arange(pairs, dtype=jnp.int32) // (TOK_DEV * TOPK)
    position = (source * CAP + rank).astype(jnp.int32)
    table = jnp.full((EXPERTS, N_EP * CAP), pairs, jnp.int32)
    return table.at[flat, position].set(jnp.arange(pairs, dtype=jnp.int32))


def reference(tokens, cotangent, mix_weights, routes, gate_proj, up_proj, down_proj):
    pairs = TOKENS * TOPK
    table = pair_table(routes)
    zero_row = jnp.zeros((1, D), jnp.bfloat16)
    token_pad = jnp.concatenate([tokens, zero_row], 0)
    back_pad = jnp.concatenate([cotangent, zero_row], 0)
    mix_pad = jnp.concatenate([mix_weights.reshape(-1), jnp.zeros((1,), jnp.bfloat16)], 0)

    def one_expert(inputs):
        ids, gate_w, up_w, down_w = inputs
        rows = token_pad[ids // TOPK]
        backs = back_pad[ids // TOPK]
        weight = mix_pad[ids].astype(jnp.float32)[:, None]
        pre_gate = jnp.dot(rows, gate_w, preferred_element_type=jnp.float32)
        pre_up = jnp.dot(rows, up_w, preferred_element_type=jnp.float32)
        active = jax.nn.silu(pre_gate)
        hidden = (active * pre_up).astype(jnp.bfloat16)
        back_hidden = lax.dot_general(backs, down_w, (((1,), (1,)), ((), ())), preferred_element_type=jnp.float32)
        pair_mix = jnp.sum(hidden.astype(jnp.float32) * back_hidden, axis=1).astype(jnp.bfloat16)
        weighted = (weight * hidden.astype(jnp.float32)).astype(jnp.bfloat16)
        down_e = lax.dot_general(weighted, backs, (((0,), (0,)), ((), ())), preferred_element_type=jnp.float32).astype(jnp.bfloat16)
        scaled = weight * back_hidden
        back_gate = (scaled * pre_up * silu_slope(pre_gate)).astype(jnp.bfloat16)
        back_up = (scaled * active).astype(jnp.bfloat16)
        gate_e = lax.dot_general(rows, back_gate, (((0,), (0,)), ((), ())), preferred_element_type=jnp.float32).astype(jnp.bfloat16)
        up_e = lax.dot_general(rows, back_up, (((0,), (0,)), ((), ())), preferred_element_type=jnp.float32).astype(jnp.bfloat16)
        count = ids.shape[0]
        split_gate = back_gate.astype(jnp.float32).reshape(count, N_TP, FF_DEV)
        split_up = back_up.astype(jnp.float32).reshape(count, N_TP, FF_DEV)
        gate_cols = gate_w.astype(jnp.float32).reshape(D, N_TP, FF_DEV)
        up_cols = up_w.astype(jnp.float32).reshape(D, N_TP, FF_DEV)
        parts = jnp.einsum('rtf,dtf->trd', split_gate, gate_cols) + jnp.einsum('rtf,dtf->trd', split_up, up_cols)
        parts = lax.optimization_barrier(parts.astype(jnp.bfloat16))
        pair_grad = jnp.sum(parts.astype(jnp.float32), axis=0).astype(jnp.bfloat16)
        return pair_grad, pair_mix, gate_e, up_e, down_e

    pair_grad, pair_mix, gate_grad, up_grad, down_grad = lax.map(one_expert, (table, gate_proj, up_proj, down_proj))
    ids = table.reshape(-1)
    summed = jnp.zeros((pairs + 1, D), jnp.float32).at[ids].add(pair_grad.reshape(-1, D).astype(jnp.float32))
    token_grad = jnp.sum(summed[:pairs].reshape(TOKENS, TOPK, D), axis=1).astype(jnp.bfloat16)
    mix_flat = jnp.zeros((pairs + 1,), jnp.bfloat16).at[ids].set(pair_mix.reshape(-1))
    mix_grad = mix_flat[:pairs].reshape(TOKENS, TOPK)
    return token_grad, mix_grad, gate_grad, up_grad, down_grad
```

```python
import jax
import jax.numpy as jnp
from jax import lax
from jax.sharding import Mesh
from jax.sharding import PartitionSpec as P

SLOTS = 5
LANES = 128


def silu_slope(pre):
    sig = jax.nn.sigmoid(pre)
    return sig * (1.0 + pre * (1.0 - sig))


def swap_cores(value):
    return lax.ppermute(value, "c", [(0, 1), (1, 0)])


def on_device(tokens, cotangent, mix_weights, routes, gate_proj, up_proj, down_proj):
    experts = lax.axis_size("ep")
    chips = lax.axis_size("x")
    core = lax.axis_index("c")
    tok_rows, width = tokens.shape
    top = routes.shape[1]
    count = experts * SLOTS
    half = width // 2
    f32 = jnp.float32
    bf16 = jnp.bfloat16

    flat = routes.T.reshape(-1)
    onehot = (flat[:, None] == jnp.arange(experts, dtype=jnp.int32)[None, :]).astype(bf16)
    pairs = tok_rows * top
    order = jnp.arange(pairs, dtype=jnp.int32)
    earlier = (order[:, None] > order[None, :]).astype(bf16)
    before = jnp.dot(earlier, onehot, preferred_element_type=f32)
    rank = jnp.sum(before * onehot.astype(f32), axis=1).astype(jnp.int32)
    target = (flat * SLOTS + rank).reshape(top, tok_rows)

    slot_ids = jnp.arange(count, dtype=jnp.int32)[:, None]
    place = jnp.zeros((count, tok_rows), bf16)
    place_mix = jnp.zeros((count, tok_rows), bf16)
    for k in range(top):
        hit = slot_ids == target[k][None, :]
        place = jnp.where(hit, jnp.asarray(1.0, bf16), place)
        place_mix = jnp.where(hit, mix_weights[:, k][None, :], place_mix)

    tok_half = lax.dynamic_slice_in_dim(tokens, core * half, half, 1)
    back_half = lax.dynamic_slice_in_dim(cotangent, core * half, half, 1)
    send_tok = jnp.dot(place, tok_half, preferred_element_type=f32).astype(bf16)
    send_back = jnp.dot(place_mix, back_half, preferred_element_type=f32).astype(bf16)
    tiles = half // LANES
    send = jnp.concatenate(
        [
            send_tok.reshape(experts, SLOTS * tiles, LANES),
            send_back.reshape(experts, SLOTS * tiles, LANES),
        ],
        axis=1,
    )
    got = lax.all_to_all(send, "ep", 0, 0, tiled=True)
    own_rows = got[:, : SLOTS * tiles].reshape(count, half)
    own_backs = got[:, SLOTS * tiles :].reshape(count, half)
    oth_rows = swap_cores(own_rows)
    oth_backs = swap_cores(own_backs)
    first = core == 0
    rows = jnp.concatenate(
        [jnp.where(first, own_rows, oth_rows), jnp.where(first, oth_rows, own_rows)], axis=1
    )
    backs = jnp.concatenate(
        [jnp.where(first, own_backs, oth_backs), jnp.where(first, oth_backs, own_backs)], axis=1
    )

    gate_w = gate_proj[0]
    up_w = up_proj[0]
    down_w = down_proj[0]
    pre_gate = jnp.dot(rows, gate_w, preferred_element_type=f32)
    pre_up = jnp.dot(rows, up_w, preferred_element_type=f32)
    active = jax.nn.silu(pre_gate)
    hidden = (active * pre_up).astype(bf16)
    scaled = lax.dot_general(backs, down_w, (((1,), (1,)), ((), ())), preferred_element_type=f32)
    mix_part = jnp.sum(hidden.astype(f32) * scaled, axis=1)
    back_gate = (scaled * pre_up * silu_slope(pre_gate)).astype(bf16)
    back_up = (scaled * active).astype(bf16)
    part = lax.dot_general(
        back_gate, gate_w, (((1,), (1,)), ((), ())), preferred_element_type=f32
    ) + lax.dot_general(back_up, up_w, (((1,), (1,)), ((), ())), preferred_element_type=f32)

    down_grad = lax.dot_general(
        hidden, backs, (((0,), (0,)), ((), ())), preferred_element_type=f32
    ).astype(bf16)
    gate_grad = lax.dot_general(
        rows, back_gate, (((0,), (0,)), ((), ())), preferred_element_type=f32
    ).astype(bf16)
    up_grad = lax.dot_general(
        rows, back_up, (((0,), (0,)), ((), ())), preferred_element_type=f32
    ).astype(bf16)

    mix_rows = jnp.pad(mix_part, (0, 8 * LANES - count)).reshape(1, 8, LANES)
    mix_rows = jnp.broadcast_to(mix_rows.astype(bf16), (chips, 8, LANES))
    part = part.astype(bf16).reshape(count, chips, 2, LANES)

    def for_core(which):
        piece = lax.dynamic_index_in_dim(part, which, 2, keepdims=False)
        return jnp.concatenate([jnp.moveaxis(piece, 1, 0), mix_rows], axis=1)

    theirs = swap_cores(for_core(1 - core))
    pair = (for_core(core).astype(f32) + theirs.astype(f32)).astype(bf16)
    pieces = lax.all_to_all(pair, "x", 0, 0, tiled=True)
    total = jnp.sum(pieces.astype(f32), axis=0).astype(bf16)
    grads = total[:count].reshape(experts, SLOTS, LANES)
    mixes = jnp.broadcast_to(total[count : count + 3][None], (experts, 3, LANES))
    back = lax.all_to_all(jnp.concatenate([grads, mixes], axis=1), "ep", 0, 0, tiled=True)

    flat_back = back.reshape(experts * 8, LANES)
    place8 = (flat * 8 + rank).reshape(top, tok_rows)
    cols = jnp.arange(experts * 8, dtype=jnp.int32)[None, :]
    pick = sum((place8[k][:, None] == cols).astype(bf16) for k in range(top))
    token_grad = jnp.dot(pick, flat_back, preferred_element_type=f32).astype(bf16)
    at = lax.axis_index("ep") * SLOTS + rank
    row8 = flat * 8 + SLOTS + at // LANES
    pick_mix = (row8[:, None] == cols).astype(bf16)
    mix_lines = jnp.dot(pick_mix, flat_back, preferred_element_type=f32)
    lane = (at % LANES)[:, None] == jnp.arange(LANES, dtype=jnp.int32)[None, :]
    mix_flat = jnp.sum(jnp.where(lane, mix_lines, 0.0), axis=1).reshape(top, tok_rows).T
    mix_grad = (mix_flat / mix_weights.astype(f32)).astype(bf16)
    return (token_grad, mix_grad, gate_grad[None], up_grad[None], down_grad[None])


def solution(mesh):
    ep = mesh.shape["ep"]
    split = Mesh(mesh.devices.reshape(ep, mesh.shape["tp"] // 2, 2), ("ep", "x", "c"))
    tp = ("x", "c")
    in_specs = (
        P("ep", None),
        P("ep", None),
        P("ep", None),
        P("ep", None),
        P("ep", None, tp),
        P("ep", None, tp),
        P("ep", tp, None),
    )
    out_specs = (
        P("ep", tp),
        P("ep", None),
        P("ep", None, tp),
        P("ep", None, tp),
        P("ep", tp, None),
    )
    return jax.shard_map(
        on_device, mesh=split, in_specs=in_specs, out_specs=out_specs, check_vma=False
    )
```

```python
import jax
import jax.numpy as jnp
from jax import lax
from jax.experimental import pallas as pl
from jax.experimental.pallas import tpu as pltpu
from jax.sharding import Mesh
from jax.sharding import PartitionSpec as P

SLOTS = 5
LANES = 128
ROWS8 = 8
F32 = jnp.float32
BF16 = jnp.bfloat16


def iota(shape, dim):
    return lax.broadcasted_iota(jnp.int32, shape, dim)


def dot_nn(a, b):
    return lax.dot_general(a, b, (((1,), (0,)), ((), ())), preferred_element_type=F32)


def dot_nt(a, b):
    return lax.dot_general(a, b, (((1,), (1,)), ((), ())), preferred_element_type=F32)


def dot_tn(a, b):
    return lax.dot_general(a, b, (((0,), (0,)), ((), ())), preferred_element_type=F32)


def swap_cores(value):
    return lax.ppermute(value, "c", [(0, 1), (1, 0)])


def slots_of(routes, experts):
    tok = routes.shape[1]
    ids = iota((experts, tok), 0)
    named = [ids == routes[k : k + 1] for k in range(2)]
    both = jnp.where(named[0] | named[1], 1.0, 0.0).astype(BF16)
    earlier = jnp.where(iota((tok, tok), 0) < iota((tok, tok), 1), 1.0, 0.0).astype(BF16)
    before = dot_nn(both, earlier)
    return [
        jnp.sum(jnp.where(hit, before, 0.0), axis=0, keepdims=True).astype(jnp.int32)
        for hit in named
    ]


def dispatch_kernel(core_ref, routes_ref, mix_ref, tok_ref, cot_ref, send_ref):
    del core_ref
    routes = routes_ref[...]
    mix = mix_ref[...].astype(F32)
    count, _ = send_ref.shape
    experts = count // (2 * SLOTS)
    tok = routes.shape[1]
    ranks = slots_of(routes, experts)
    at = [routes[k : k + 1] * (2 * SLOTS) + ranks[k] for k in range(2)]
    row = iota((count, tok), 0)
    place = jnp.where((row == at[0]) | (row == at[1]), 1.0, 0.0)
    scale = jnp.where(
        row == at[0] + SLOTS, mix[0:1], jnp.where(row == at[1] + SLOTS, mix[1:2], 0.0)
    )
    pick = jnp.concatenate([place.astype(BF16), scale.astype(BF16)], axis=1)
    source = jnp.concatenate([tok_ref[...], cot_ref[...]], axis=0)
    send_ref[...] = dot_nn(pick, source).astype(BF16)


def fetch_kernel(gate_ref, up_ref, down_ref, pair_ref, down_out_ref):
    pair_ref[:, :LANES] = gate_ref[...]
    pair_ref[:, LANES:] = up_ref[...]
    down_out_ref[...] = down_ref[...]


def forward_kernel(
    core_ref, own_t, oth_t, own_b, oth_b, pair_ref, down_ref, near_ref, far_ref, acts_ref
):
    core = core_ref[0]
    half = own_t.shape[1]
    count = own_t.shape[0]
    chips = near_ref.shape[0]
    mine = pl.ds(pl.multiple_of(core * half, half), half)
    other = pl.ds(pl.multiple_of((1 - core) * half, half), half)
    pre = dot_nn(own_t[...], pair_ref[mine, :]) + dot_nn(oth_t[...], pair_ref[other, :])
    scaled = dot_nt(own_b[...], down_ref[:, mine]) + dot_nt(oth_b[...], down_ref[:, other])
    pre_gate = pre[:, :LANES]
    pre_up = pre[:, LANES:]
    sig = jax.nn.sigmoid(pre_gate)
    active = pre_gate * sig
    hidden = (active * pre_up).astype(BF16)
    back_gate = (scaled * pre_up * (sig * (1.0 + pre_gate * (1.0 - sig)))).astype(BF16)
    back_up = (scaled * active).astype(BF16)
    acts_ref[0] = hidden
    acts_ref[1] = back_gate
    acts_ref[2] = back_up

    mix = jnp.sum(hidden.astype(F32) * scaled, axis=1, keepdims=True)
    slot = iota((count, LANES), 0)
    spread = jnp.where(iota((count, LANES), 1) == slot % LANES, mix, 0.0)
    lines = [
        jnp.sum(jnp.where(slot // LANES == k, spread, 0.0), axis=0, keepdims=True)
        for k in range(pl.cdiv(count, LANES))
    ]
    lines += [jnp.zeros((1, LANES), F32)] * (ROWS8 - len(lines))
    table = jnp.concatenate(lines, axis=0)

    backs = jnp.concatenate([back_gate, back_up], axis=1)
    for chip in range(chips):
        for which, out in ((core, near_ref), (1 - core, far_ref)):
            cols = pl.ds(pl.multiple_of((2 * chip + which) * LANES, LANES), LANES)
            part = dot_nt(backs, pair_ref[cols, :])
            out[chip, 0:count, :] = part.astype(out.dtype)
            out[chip, count : count + ROWS8, :] = table.astype(out.dtype)


def weights_kernel(core_ref, own_t, oth_t, own_b, oth_b, acts_ref, gate_ref, up_ref, down_ref):
    core = core_ref[0]
    half = own_t.shape[1]
    mine = pl.ds(pl.multiple_of(core * half, half), half)
    other = pl.ds(pl.multiple_of((1 - core) * half, half), half)
    backs = jnp.concatenate([acts_ref[1], acts_ref[2]], axis=1)
    hidden = acts_ref[0]
    for where, rows, cots in ((mine, own_t, own_b), (other, oth_t, oth_b)):
        grads = dot_tn(rows[...], backs)
        gate_ref[where, :] = grads[:, :LANES].astype(BF16)
        up_ref[where, :] = grads[:, LANES:].astype(BF16)
        down_ref[:, where] = dot_tn(hidden, cots[...]).astype(BF16)


def gather_kernel(pieces_ref, back_ref):
    total = pieces_ref[0].astype(F32)
    for k in range(1, pieces_ref.shape[0]):
        total = total + pieces_ref[k].astype(F32)
    total = total.astype(BF16)
    rows = back_ref.shape[0]
    count = rows // ROWS8 * SLOTS
    row = iota((rows, total.shape[0]), 0)
    slot = row % ROWS8
    source = jnp.where(slot < SLOTS, row // ROWS8 * SLOTS + slot, count + slot - SLOTS)
    pick = jnp.where(iota((rows, total.shape[0]), 1) == source, 1.0, 0.0).astype(BF16)
    back_ref[...] = dot_nn(pick, total).astype(BF16)


def combine_kernel(block_ref, routes_ref, mix_ref, back_ref, token_ref, mix_out_ref):
    routes = routes_ref[...]
    mix = mix_ref[...].astype(F32)
    back = back_ref[...]
    rows = back.shape[0]
    tok = routes.shape[1]
    ranks = slots_of(routes, rows // ROWS8)
    row = iota((rows, tok), 0)
    at = [routes[k : k + 1] * ROWS8 + ranks[k] for k in range(2)]
    pick = jnp.where((row == at[0]) | (row == at[1]), 1.0, 0.0).astype(BF16)
    token_ref[...] = dot_tn(pick, back).astype(BF16)
    for k in range(2):
        slot = block_ref[0] * SLOTS + ranks[k]
        line = routes[k : k + 1] * ROWS8 + SLOTS + slot // LANES
        pick = jnp.where(row == line, 1.0, 0.0).astype(BF16)
        lines = dot_tn(back, pick)
        found = jnp.where(iota((LANES, tok), 0) == slot % LANES, lines, 0.0)
        value = jnp.sum(found, axis=0, keepdims=True) / mix[k : k + 1]
        mix_out_ref[k : k + 1, :] = value.astype(BF16)


def in_hbm(value):
    return pltpu.with_memory_space_constraint(value, pltpu.HBM)


def params():
    return pltpu.CompilerParams(vmem_limit_bytes=24 * 1024 * 1024)


def smem():
    return pl.BlockSpec(memory_space=pltpu.SMEM)


def vmem():
    return pl.BlockSpec(memory_space=pltpu.VMEM)


def call(kernel, out_shape, n_in, cost=None, name=None, scalars=1):
    outs = out_shape if isinstance(out_shape, tuple) else (out_shape,)
    specs = tuple(vmem() for _ in outs)
    return pl.pallas_call(
        kernel,
        out_shape=out_shape,
        in_specs=[smem()] * scalars + [vmem()] * n_in,
        out_specs=specs if isinstance(out_shape, tuple) else specs[0],
        cost_estimate=cost,
        compiler_params=params(),
        name=name,
    )


def on_device(tokens, cotangent, mix_weights, routes, gate_proj, up_proj, down_proj):
    experts = lax.axis_size("ep")
    chips = lax.axis_size("x")
    core = lax.axis_index("c").astype(jnp.int32).reshape(1)
    block = lax.axis_index("ep").astype(jnp.int32).reshape(1)
    tok_rows, width = tokens.shape
    count = experts * SLOTS
    half = width // 2
    tiles = half // LANES
    struct = jax.ShapeDtypeStruct
    routes_t = routes.T
    mix_t = mix_weights.T
    gate_w = gate_proj[0]
    up_w = up_proj[0]
    down_w = down_proj[0]

    send = pl.pallas_call(
        dispatch_kernel,
        out_shape=struct((2 * count, half), BF16),
        grid_spec=pltpu.PrefetchScalarGridSpec(
            num_scalar_prefetch=1,
            grid=(1,),
            in_specs=[
                pl.BlockSpec(routes_t.shape, lambda i, c: (0, 0)),
                pl.BlockSpec(mix_t.shape, lambda i, c: (0, 0)),
                pl.BlockSpec((tok_rows, half), lambda i, c: (0, c[0])),
                pl.BlockSpec((tok_rows, half), lambda i, c: (0, c[0])),
            ],
            out_specs=pl.BlockSpec((2 * count, half), lambda i, c: (0, 0)),
        ),
        compiler_params=params(),
        name="dispatch",
    )(core, *(in_hbm(a) for a in (routes_t, mix_t, tokens, cotangent)))
    send = send.reshape(experts, 2 * SLOTS * tiles, LANES)
    got = lax.all_to_all(send, "ep", 0, 0, tiled=True)
    own_t = got[:, : SLOTS * tiles].reshape(count, half)
    own_b = got[:, SLOTS * tiles :].reshape(count, half)
    oth_t = swap_cores(own_t)
    oth_b = swap_cores(own_b)
    gate_w, up_w, down_w, _ = lax.optimization_barrier((gate_w, up_w, down_w, got))
    pair_w, down_w = call(
        fetch_kernel,
        (pltpu.VMEM((width, 2 * LANES), BF16), pltpu.VMEM(down_w.shape, BF16)),
        3,
        name="fetch",
        scalars=0,
    )(*(in_hbm(w) for w in (gate_w, up_w, down_w)))

    shape = (chips, count + ROWS8, LANES)
    near, far, acts = call(
        forward_kernel,
        (struct(shape, F32), struct(shape, BF16), struct((3, count, LANES), BF16)),
        6,
        name="forward",
    )(core, own_t, oth_t, own_b, oth_b, pair_w, down_w)
    theirs = swap_cores(far)
    pair = (near + theirs.astype(F32)).astype(BF16)
    pieces = lax.all_to_all(pair, "x", 0, 0, tiled=True)
    back = pl.pallas_call(
        gather_kernel,
        out_shape=struct((experts * ROWS8, LANES), BF16),
        compiler_params=params(),
        name="gather",
    )(pieces)
    acts, back = lax.optimization_barrier((acts, back))
    gate_grad, up_grad, down_grad = call(
        weights_kernel,
        (struct((width, LANES), BF16), struct((width, LANES), BF16), struct((LANES, width), BF16)),
        5,
        cost=pl.CostEstimate(
            flops=6 * count * width * LANES, bytes_accessed=6 * width * LANES, transcendentals=0
        ),
        name="weights",
    )(core, own_t, oth_t, own_b, oth_b, acts)
    back = lax.all_to_all(back.reshape(experts, ROWS8, LANES), "ep", 0, 0, tiled=True)
    token_grad, mix_grad = call(
        combine_kernel,
        (struct((tok_rows, LANES), BF16), struct(mix_t.shape, BF16)),
        3,
        name="combine",
    )(block, routes_t, mix_t, back.reshape(experts * ROWS8, LANES))
    return (token_grad, mix_grad.T, gate_grad[None], up_grad[None], down_grad[None])


def solution(mesh):
    ep = mesh.shape["ep"]
    split = Mesh(mesh.devices.reshape(ep, mesh.shape["tp"] // 2, 2), ("ep", "x", "c"))
    tp = ("x", "c")
    in_specs = (
        P("ep", None),
        P("ep", None),
        P("ep", None),
        P("ep", None),
        P("ep", None, tp),
        P("ep", None, tp),
        P("ep", tp, None),
    )
    out_specs = (
        P("ep", tp),
        P("ep", None),
        P("ep", None, tp),
        P("ep", None, tp),
        P("ep", tp, None),
    )
    return jax.shard_map(
        on_device, mesh=split, in_specs=in_specs, out_specs=out_specs, check_vma=False
    )
```

```python
import functools

import jax
import jax.numpy as jnp
from jax import lax
from jax.experimental import pallas as pl
from jax.experimental.pallas import tpu as pltpu
from jax.sharding import Mesh
from jax.sharding import PartitionSpec as P


SLOTS = 5
PART = 3
LANES = 128
ROWS8 = 8
F32 = jnp.float32
BF16 = jnp.bfloat16


def iota(shape, dim):
    return lax.broadcasted_iota(jnp.int32, shape, dim)


def dot_nn(a, b):
    return lax.dot_general(a, b, (((1,), (0,)), ((), ())), preferred_element_type=F32)


def dot_nt(a, b):
    return lax.dot_general(a, b, (((1,), (1,)), ((), ())), preferred_element_type=F32)


def dot_tn(a, b):
    return lax.dot_general(a, b, (((0,), (0,)), ((), ())), preferred_element_type=F32)


def swap_cores(value):
    return lax.ppermute(value, "c", [(0, 1), (1, 0)])


def slots_of(routes, experts):
    tok = routes.shape[1]
    ids = iota((experts, tok), 0)
    named = [ids == routes[k : k + 1] for k in range(2)]
    both = jnp.where(named[0] | named[1], 1.0, 0.0).astype(BF16)
    earlier = jnp.where(iota((tok, tok), 0) < iota((tok, tok), 1), 1.0, 0.0).astype(BF16)
    before = dot_nn(both, earlier)
    return [
        jnp.sum(jnp.where(hit, before, 0.0), axis=0, keepdims=True).astype(jnp.int32)
        for hit in named
    ]


def dispatch_kernel(place_ref, routes_ref, mix_ref, tok_ref, cot_ref, send_ref):
    routes = routes_ref[...]
    mix = mix_ref[...].astype(F32)
    experts = send_ref.shape[0]
    count = experts * 2 * PART
    tok = routes.shape[1]
    ranks = slots_of(routes, experts)
    first = place_ref[1] * PART
    at = []
    for k in range(2):
        slot = ranks[k] - first
        kept = (slot >= 0) & (slot < PART)
        at.append(jnp.where(kept, routes[k : k + 1] * (2 * PART) + slot, -count))
    row = iota((count, tok), 0)
    place = jnp.where((row == at[0]) | (row == at[1]), 1.0, 0.0)
    scale = jnp.where(
        row == at[0] + PART, mix[0:1], jnp.where(row == at[1] + PART, mix[1:2], 0.0)
    )
    pick = jnp.concatenate([place.astype(BF16), scale.astype(BF16)], axis=1)
    source = jnp.concatenate([tok_ref[...], cot_ref[...]], axis=0)
    send_ref[...] = dot_nn(pick, source).astype(BF16).reshape(send_ref.shape)


def unpacked(wire_ref):
    experts, lines, _ = wire_ref.shape
    cut = lines // 2
    shape = (experts * PART, cut // PART * LANES)
    return wire_ref[:, :cut, :].reshape(shape), wire_ref[:, cut:, :].reshape(shape)


def unpack_kernel(wire_ref, mark_ref, gate_hbm, up_hbm, down_hbm, *refs):
    del mark_ref
    rows_ref, cots_ref, gate_ref, up_ref, down_ref, sems = refs
    pairs = ((gate_hbm, gate_ref), (up_hbm, up_ref), (down_hbm, down_ref))
    copies = [pltpu.make_async_copy(a, b, sems.at[k]) for k, (a, b) in enumerate(pairs)]
    for copy in copies:
        copy.start()
    rows_ref[...], cots_ref[...] = unpacked(wire_ref)
    for copy in copies:
        copy.wait()


def mark_kernel(core_ref, out_ref):
    out_ref[...] = jnp.zeros(out_ref.shape, F32) + core_ref[0].astype(F32)


def forward_kernel(place_ref, own_t, own_b, wire_ref, *refs):
    weights = (refs[0:3], refs[3:6])
    near_ref, far_ref, acts_ref, oth_t, oth_b = refs[6:]
    oth_t[...], oth_b[...] = unpacked(wire_ref)
    core = place_ref[0]
    count, half = own_t.shape
    chips = near_ref.shape[0]
    mine = pl.ds(pl.multiple_of(core * half, half), half)
    other = pl.ds(pl.multiple_of((1 - core) * half, half), half)

    backs = []
    mix = jnp.zeros((count, 1), F32)
    for k, (gate_ref, up_ref, down_ref) in enumerate(weights):
        pre = sum(
            dot_nn(rows[...], jnp.concatenate([gate_ref[where, :], up_ref[where, :]], axis=1))
            for rows, where in ((own_t, mine), (oth_t, other))
        )
        scaled = dot_nt(own_b[...], down_ref[:, mine]) + dot_nt(oth_b[...], down_ref[:, other])
        pre_gate = pre[:, :LANES]
        pre_up = pre[:, LANES:]
        sig = jax.nn.sigmoid(pre_gate)
        active = pre_gate * sig
        hidden = (active * pre_up).astype(BF16)
        back_gate = (scaled * pre_up * (sig * (1.0 + pre_gate * (1.0 - sig)))).astype(BF16)
        back_up = (scaled * active).astype(BF16)
        acts_ref[k, 0] = hidden
        acts_ref[k, 1] = back_gate
        acts_ref[k, 2] = back_up
        backs += [back_gate, back_up]
        mix = mix + jnp.sum(hidden.astype(F32) * scaled, axis=1, keepdims=True)

    row = iota((count, LANES), 0)
    source = (row * 171) >> 9
    slot = source * SLOTS + place_ref[1] * PART + (row - source * PART)
    spread = jnp.where(iota((count, LANES), 1) == slot % LANES, mix, 0.0)
    lines = [
        jnp.sum(jnp.where(slot // LANES == k, spread, 0.0), axis=0, keepdims=True)
        for k in range(ROWS8 - SLOTS)
    ]
    lines += [jnp.zeros((1, LANES), F32)] * SLOTS
    table = jnp.concatenate(lines, axis=0)

    backs = jnp.concatenate(backs, axis=1)
    for chip in range(chips):
        for which, out in ((core, near_ref), (1 - core, far_ref)):
            cols = pl.ds(pl.multiple_of((2 * chip + which) * LANES, LANES), LANES)
            rhs = jnp.concatenate([w[cols, :] for g in weights for w in g[:2]], axis=1)
            out[chip, 0:count, :] = dot_nt(backs, rhs).astype(out.dtype)
            out[chip, count : count + ROWS8, :] = table.astype(out.dtype)


def weights_kernel(which, place_ref, own_t, oth_t, own_b, oth_b, acts_ref, *outs):
    gate_ref, up_ref, down_ref = outs
    core = place_ref[0]
    half = own_t.shape[1]
    mine = pl.ds(pl.multiple_of(core * half, half), half)
    other = pl.ds(pl.multiple_of((1 - core) * half, half), half)
    backs = jnp.concatenate([acts_ref[which, 1], acts_ref[which, 2]], axis=1)
    hidden = acts_ref[which, 0]
    for where, rows, cots in ((mine, own_t, own_b), (other, oth_t, oth_b)):
        grads = dot_tn(rows[...], backs)
        gate_ref[where, :] = grads[:, :LANES].astype(gate_ref.dtype)
        up_ref[where, :] = grads[:, LANES:].astype(up_ref.dtype)
        down_ref[:, where] = dot_tn(hidden, cots[...]).astype(down_ref.dtype)


def add_kernel(*refs):
    for own, got, out in zip(refs[0:3], refs[3:6], refs[6:9]):
        out[...] = (own[...] + got[...].astype(F32)).astype(out.dtype)


def gather_kernel(pieces_ref, back_ref):
    chips, lines, _ = pieces_ref.shape
    count = lines - ROWS8
    sums = []
    for parity in range(2):
        total = pieces_ref[parity].astype(F32)
        for k in range(parity + 2, chips, 2):
            total = total + pieces_ref[k].astype(F32)
        sums.append(total)
    table = sums[0][count:] + sums[1][count:]
    total = jnp.concatenate([sums[0][:count], sums[1][:count], table], axis=0).astype(BF16)
    rows = back_ref.shape[0]
    row = iota((rows, total.shape[0]), 0)
    source = (row >> 3) * PART
    slot = row & 7
    source = jnp.where(
        slot < PART,
        source + slot,
        jnp.where(slot < SLOTS, count + source + slot - PART, 2 * count + slot - SLOTS),
    )
    pick = jnp.where(iota((rows, total.shape[0]), 1) == source, 1.0, 0.0).astype(BF16)
    back_ref[...] = dot_nn(pick, total).astype(BF16)


def combine_kernel(block_ref, routes_ref, mix_ref, back_ref, token_ref, mix_out_ref):
    routes = routes_ref[...]
    mix = mix_ref[...].astype(F32)
    back = back_ref[...]
    rows = back.shape[0]
    tok = routes.shape[1]
    ranks = slots_of(routes, rows // ROWS8)
    row = iota((rows, tok), 0)
    at = [routes[k : k + 1] * ROWS8 + ranks[k] for k in range(2)]
    pick = jnp.where((row == at[0]) | (row == at[1]), 1.0, 0.0).astype(BF16)
    token_ref[...] = dot_tn(pick, back).astype(BF16)
    for k in range(2):
        slot = block_ref[0] * SLOTS + ranks[k]
        line = routes[k : k + 1] * ROWS8 + SLOTS + slot // LANES
        pick = jnp.where(row == line, 1.0, 0.0).astype(BF16)
        lines = dot_tn(back, pick)
        found = jnp.where(iota((LANES, tok), 0) == slot % LANES, lines, 0.0)
        value = jnp.sum(found, axis=0, keepdims=True) / mix[k : k + 1]
        mix_out_ref[k : k + 1, :] = value.astype(BF16)


def in_hbm(value):
    return pltpu.with_memory_space_constraint(value, pltpu.HBM)


def params():
    return pltpu.CompilerParams(vmem_limit_bytes=24 * 1024 * 1024)


def smem():
    return pl.BlockSpec(memory_space=pltpu.SMEM)


def vmem():
    return pl.BlockSpec(memory_space=pltpu.VMEM)


def call(kernel, out_shape, n_in, cost=None, scalars=1, n_hbm=0, scratch=()):
    outs = out_shape if isinstance(out_shape, tuple) else (out_shape,)
    specs = tuple(vmem() for _ in outs)
    return pl.pallas_call(
        kernel,
        out_shape=out_shape,
        in_specs=[smem()] * scalars + [vmem()] * n_in + [pl.BlockSpec(memory_space=pl.ANY)] * n_hbm,
        scratch_shapes=scratch,
        out_specs=specs if isinstance(out_shape, tuple) else specs[0],
        cost_estimate=cost,
        compiler_params=params(),
    )


def on_device(tokens, cotangent, mix_weights, routes, gate_proj, up_proj, down_proj):
    experts = lax.axis_size("ep")
    chips = lax.axis_size("x")
    place = jnp.stack([lax.axis_index("c"), lax.axis_index("x") & 1]).astype(jnp.int32)
    block = lax.axis_index("ep").astype(jnp.int32).reshape(1)
    tok_rows, width = tokens.shape
    count = experts * PART
    half = width // 2
    wire = (experts, 2 * PART * half // LANES, LANES)
    struct = jax.ShapeDtypeStruct
    routes_t = routes.T
    mix_t = mix_weights.T
    own_w = (gate_proj[0], up_proj[0], down_proj[0])

    lend = []
    for k in range(chips):
        lend += [(2 * k, 2 * ((k - 1) % chips)), (2 * k + 1, 2 * ((k + 1) % chips) + 1)]
    give_back = [(b, a) for a, b in lend]

    send = pl.pallas_call(
        dispatch_kernel,
        out_shape=struct(wire, BF16),
        grid_spec=pltpu.PrefetchScalarGridSpec(
            num_scalar_prefetch=1,
            grid=(1,),
            in_specs=[
                pl.BlockSpec(routes_t.shape, lambda i, c: (0, 0)),
                pl.BlockSpec(mix_t.shape, lambda i, c: (0, 0)),
                pl.BlockSpec((tok_rows, half), lambda i, c: (0, c[0])),
                pl.BlockSpec((tok_rows, half), lambda i, c: (0, c[0])),
            ],
            out_specs=pl.BlockSpec(wire, lambda i, c: (0, 0, 0)),
        ),
        compiler_params=params(),
        name="dispatch",
    )(place, *(in_hbm(a) for a in (routes_t, mix_t, tokens, cotangent)))
    got = lax.all_to_all(send, "ep", 0, 0, tiled=True)
    lent_w = tuple(lax.ppermute(w, ("x", "c"), lend) for w in own_w)
    mark = call(mark_kernel, struct((8, LANES), F32), 0)(place)
    theirs = swap_cores(got)
    rows = struct((count, half), BF16)
    in_vmem = [pltpu.VMEM(w.shape, BF16) for w in own_w]
    copies = pltpu.SemaphoreType.DMA((3,))
    own_t, own_b, *held_w = call(
        unpack_kernel, (rows, rows, *in_vmem), 2, scalars=0, n_hbm=3, scratch=(copies,)
    )(got, mark, *(in_hbm(w) for w in own_w))

    shape = (chips, count + ROWS8, LANES)
    near, far, acts, oth_t, oth_b = call(
        forward_kernel,
        (struct(shape, F32), struct(shape, BF16), struct((2, 3, count, LANES), BF16), rows, rows),
        9,
    )(place, own_t, own_b, theirs, *held_w, *lent_w)
    theirs = swap_cores(far)
    pair = (near + theirs.astype(F32)).astype(BF16)
    pieces = lax.all_to_all(pair, "x", 0, 0, tiled=True)

    shapes = ((width, LANES), (width, LANES), (LANES, width))
    cost = pl.CostEstimate(
        flops=6 * count * width * LANES, bytes_accessed=6 * width * LANES, transcendentals=0
    )
    grads = [
        call(
            functools.partial(weights_kernel, k),
            tuple(pltpu.VMEM(s, F32 if k == 0 else BF16) for s in shapes),
            5,
            cost=cost,
        )(place, own_t, oth_t, own_b, oth_b, acts)
        for k in (1, 0)
    ]
    given = tuple(lax.ppermute(g, ("x", "c"), give_back) for g in grads[0])

    back = pl.pallas_call(
        gather_kernel,
        out_shape=struct((experts * ROWS8, LANES), BF16),
        compiler_params=params(),
        name="gather",
    )(pieces)
    back = lax.all_to_all(back.reshape(experts, ROWS8, LANES), "ep", 0, 0, tiled=True)
    token_grad, mix_grad = call(
        combine_kernel, (struct((tok_rows, LANES), BF16), struct(mix_t.shape, BF16)), 3
    )(block, routes_t, mix_t, back.reshape(experts * ROWS8, LANES))
    gate_grad, up_grad, down_grad = call(
        add_kernel, tuple(struct(s, BF16) for s in shapes), 6, scalars=0
    )(*grads[1], *given)
    return (token_grad, mix_grad.T, gate_grad[None], up_grad[None], down_grad[None])


def solution(mesh):
    ep = mesh.shape["ep"]
    split = Mesh(mesh.devices.reshape(ep, mesh.shape["tp"] // 2, 2), ("ep", "x", "c"))
    tp = ("x", "c")
    in_specs = (
        P("ep", None),
        P("ep", None),
        P("ep", None),
        P("ep", None),
        P("ep", None, tp),
        P("ep", None, tp),
        P("ep", tp, None),
    )
    out_specs = (
        P("ep", tp),
        P("ep", None),
        P("ep", None, tp),
        P("ep", None, tp),
        P("ep", tp, None),
    )
    return jax.shard_map(
        on_device, mesh=split, in_specs=in_specs, out_specs=out_specs, check_vma=False
    )
```
